32 devices in a mesh: grp: 2 (over y), tp: 4 (over z), dp: 4 (over x, core).
Axes of the slice: x: 2, y: 2, z: 4, core: 2. Of those that a mesh axis runs over, the one named last changes fastest.
Arguments:
- hidden_in: bfloat16 [96, 4096], P(('grp', 'tp'), 'dp'), parts along dimension 0, may hold values from -40 to 40
- input_norm_gain: float32 [2, 4096], P(None, 'dp'), may hold values from 0.1 to 1.9
- w_query: bfloat16 [2, 4096, 2048], P(None, 'dp', 'tp'), may hold values from -0.09375 to 0.09375
- w_key: bfloat16 [2, 4096, 2048], P(None, 'dp', 'tp'), may hold values from -0.09375 to 0.09375
- w_decay: bfloat16 [2, 4096, 2048], P(None, 'dp', 'tp'), may hold values from -0.375 to 0.375
- w_value: bfloat16 [2, 4096, 4096], P(None, 'dp', 'tp'), may hold values from -0.09375 to 0.09375
- w_gate: bfloat16 [2, 4096, 4096], P(None, 'dp', 'tp'), may hold values from -0.09375 to 0.09375
- out_gain: float32 [2, 4096], P(None, 'tp'), may hold values from 0.1 to 1.9
- w_out: bfloat16 [2, 4096, 4096], P(None, 'tp', 'dp'), may hold values from -0.09375 to 0.09375
- decay_offset: float32 [2, 96, 2048], P(None, ('grp', 'dp'), 'tp'), parts along dimension 1, may hold values from -0.7 to 0
- state: float32 [2, 96, 32, 64, 128], P(None, ('grp', 'dp'), 'tp'), parts along dimension 1, may hold values from -3 to 3
Outputs:
- hidden_out: bfloat16 [96, 4096], P(('grp', 'tp'), 'dp'), parts along dimension 0
- new_state: float32 [2, 96, 32, 64, 128], P(None, ('grp', 'dp'), 'tp'), parts along dimension 1
The draws below stay inside these ranges and needn't reach their ends.
There are 2 independent parts, one for each index of `grp`. The reference program is written for one: setup_inputs(seed, part) draws one part's arguments, and reference() takes and returns one part's arrays. A program takes and returns all parts, laid end to end along the dimension named above; an argument that names none is the same for every part. Nothing has to cross between parts.
All inputs are finite; a program needn't handle non-finite values.
Results may differ from the reference program's by a relative error of at most 0.017.
Values may be sent and summed in bfloat16 or wider, within the bound.
A program may use at most 64 MiB of HBM per device.

```python
import jax
import jax.numpy as jnp
from jax import lax

D = 4096
HEADS = 32
HEAD_KEY = 64
VALUE_CHANNELS = 128
LAYERS = 2
BATCH = 48
KEY_W = 2048
VAL_W = 4096
N_DP = 4


def draw_hidden_in(key, part):
    base_key, column_key, row_key = jax.random.split(key, 3)
    column = jnp.arange(D, dtype=jnp.float32) / (D - 1)
    column_scale = jnp.exp(jnp.log(3.0) * column + jax.random.uniform(column_key, (D,), jnp.float32, -0.5, 0.5))
    values = jnp.clip(jax.random.normal(base_key, (BATCH, D), jnp.float32), -4.0, 4.0)
    row_scale = jnp.exp(jax.random.uniform(row_key, (BATCH, 1), jnp.float32, -0.7, 0.7))
    return (values * row_scale * column_scale[None, :]).astype(jnp.bfloat16)


def level_of(own_key, extent, shards, low, largest):
    level = 1.0
    for position, blocks in shards:
        steps = jax.random.uniform(jax.random.fold_in(jax.random.fold_in(own_key, 6), position), (blocks,), jnp.float32, low / len(shards), largest / len(shards))
        level = level * jnp.repeat(jnp.exp(steps), extent[position] // blocks).reshape((-1,) + (1,) * (len(extent) - 1 - position))
    return level


def bell_draw(stream_key, dims, scale, bound, cuts=(), kind=jnp.bfloat16):
    result = scale * jax.random.normal(stream_key, dims, jnp.float32)
    if cuts:
        result = result * level_of(stream_key, dims, cuts, -0.22, 0.18)
    return jnp.clip(result, -bound, bound).astype(kind)


def setup_inputs(seed: int = 0, part: int = 0) -> dict:
    arg_keys = jax.random.split(jax.random.key(seed), 12)
    part_keys = jax.random.split(jax.random.fold_in(arg_keys[11], part), 12)
    hidden_in = draw_hidden_in(jax.random.fold_in(jax.random.fold_in(arg_keys[11], part), 71), part)
    input_norm_gain = jnp.clip(1.0 + 0.18 * jax.random.normal(arg_keys[1], (LAYERS, D), jnp.float32), 0.1, 1.9)
    w_query = bell_draw(arg_keys[2], (LAYERS, D, KEY_W), D ** -0.5, 0.09375, ((1, 4), (2, 4)))
    w_key = bell_draw(arg_keys[3], (LAYERS, D, KEY_W), D ** -0.5, 0.09375, ((1, 4), (2, 4)))
    w_decay = bell_draw(arg_keys[4], (LAYERS, D, KEY_W), (D // 16) ** -0.5, 0.375, ((1, 4), (2, 4)))
    w_value = bell_draw(arg_keys[5], (LAYERS, D, VAL_W), D ** -0.5, 0.09375, ((1, 4), (2, 4)))
    w_gate = bell_draw(arg_keys[6], (LAYERS, D, VAL_W), D ** -0.5, 0.09375, ((1, 4), (2, 4)))
    out_gain = jnp.clip(1.0 + 0.18 * jax.random.normal(arg_keys[7], (LAYERS, VAL_W), jnp.float32), 0.1, 1.9)
    w_out = bell_draw(arg_keys[8], (LAYERS, VAL_W, D), VAL_W ** -0.5, 0.09375, ((1, 4), (2, 4)))
    decay_offset = jnp.clip(-0.7 + 0.7 * jax.random.uniform(part_keys[9], (LAYERS, BATCH, KEY_W), jnp.float32) ** level_of(part_keys[9], (LAYERS, BATCH, KEY_W), ((1, 4), (2, 4)), -0.2, 0.2), -0.7, 0.0)
    state = bell_draw(part_keys[10], (LAYERS, BATCH, HEADS, HEAD_KEY, VALUE_CHANNELS), 0.5, 3.0, ((1, 4), (2, 4)), jnp.float32)
    return dict(hidden_in=hidden_in, input_norm_gain=input_norm_gain, w_query=w_query, w_key=w_key, w_decay=w_decay, w_value=w_value, w_gate=w_gate, out_gain=out_gain, w_out=w_out, decay_offset=decay_offset, state=state)


epsilon = 1e-06
softness_factor = 16.0

def reference(hidden_in, input_norm_gain, w_query, w_key, w_decay, w_value, w_gate, out_gain, w_out, decay_offset, state):
    hidden = hidden_in
    states = []
    for index_of_block in range(LAYERS):
        widened = hidden.astype(jnp.float32)
        squares = lax.optimization_barrier(jnp.sum(widened * widened, axis=1))
        scaled_query = (widened * input_norm_gain[index_of_block][None, :]).astype(jnp.bfloat16)
        groups = scaled_query.astype(jnp.float32).reshape(BATCH, N_DP, D // N_DP)
        pieces = []
        for matrix in (w_query, w_key, w_decay, w_value, w_gate):
            blocks = matrix[index_of_block].astype(jnp.float32).reshape(N_DP, D // N_DP, matrix.shape[2])
            partial_value = jnp.einsum('bnr,nrc->nbc', groups, blocks, precision=lax.Precision.HIGHEST)
            rounded = lax.optimization_barrier(partial_value.astype(jnp.bfloat16))
            pieces.append(lax.optimization_barrier(jnp.sum(rounded.astype(jnp.float32), axis=0)))
        inverse = lax.rsqrt(squares / D + epsilon)[:, None]
        query_rows = (pieces[0] * inverse).reshape(BATCH, HEADS, HEAD_KEY)
        key_rows = (pieces[1] * inverse).reshape(BATCH, HEADS, HEAD_KEY) * HEAD_KEY ** (-0.5)
        decay_logits = pieces[2] * inverse
        value_rows = (pieces[3] * inverse).reshape(BATCH, HEADS, VALUE_CHANNELS)
        gate_rows = (pieces[4] * inverse).reshape(BATCH, HEADS, VALUE_CHANNELS)
        decay_logarithm = jax.nn.log_sigmoid(decay_logits) / softness_factor + decay_offset[index_of_block]
        decay_rate = jnp.exp(decay_logarithm).reshape(BATCH, HEADS, HEAD_KEY)
        fresh = decay_rate[:, :, :, None] * state[index_of_block] + key_rows[:, :, :, None] * value_rows[:, :, None, :]
        readout = lax.optimization_barrier(jnp.sum(query_rows[:, :, :, None] * fresh, axis=2))
        normed = readout * lax.rsqrt(lax.optimization_barrier(jnp.mean(readout * readout, axis=2, keepdims=True)) + epsilon)
        normed = normed * out_gain[index_of_block].reshape(HEADS, VALUE_CHANNELS)[None]
        gated_out = (normed * jax.nn.silu(gate_rows)).reshape(BATCH, VAL_W).astype(jnp.bfloat16)
        mixed = jnp.dot(gated_out, w_out[index_of_block], preferred_element_type=jnp.float32)
        hidden = (widened + mixed).astype(jnp.bfloat16)
        states.append(fresh)
    return (hidden, jnp.stack(states))
```

```python
import functools

import jax
import jax.numpy as jnp
from jax import lax
from jax.experimental import pallas as pl
from jax.experimental.pallas import tpu as pltpu
from jax.sharding import PartitionSpec as P

EPSILON = 1e-06
SOFTNESS = 16.0
F32 = jnp.float32
BF16 = jnp.bfloat16


def block_kernel(
    n_tp, n_dp, d_model, head_key, value_channels,
    hidden_ref, gain_ref, out_gain_ref, offset_ref,
    wq_hbm, wk_hbm, wd_hbm, wv_hbm, wg_hbm, wo_hbm, state_hbm,
    hidden_out_ref, new_state_ref,
    wq, wk, wd, wv, wg, wo, state,
    current, gathered, part_send, part_recv, sq_send, sq_recv,
    turned, products, value_buf, gate_buf, decay_buf, readout,
    gated_all, mix_send, mix_recv,
    load_sem, gather_sems, part_sems, sq_sems, gated_sems, mix_sems,
):
    layers, rows, heads = state.shape[0], state.shape[1], state.shape[2]
    pad = current.shape[1]
    width = current.shape[2]
    pieces, piece = part_send.shape[1], part_send.shape[4]
    mix_pieces, mix_piece = mix_send.shape[1], mix_send.shape[4]
    key_cols = heads * head_key
    value_cols = heads * value_channels
    tp = lax.axis_index("tp")
    dp = lax.axis_index("dp")

    sources = (wq_hbm, wk_hbm, wd_hbm, wv_hbm, wg_hbm, wo_hbm, state_hbm)
    targets = (wq, wk, wd, wv, wg, wo, state)

    def load(index, layer):
        return pltpu.make_async_copy(
            sources[index].at[layer], targets[index].at[layer], load_sem.at[index, layer]
        )

    for layer in range(layers):
        for index in (0, 1, 2, 3, 4, 6, 5):
            load(index, layer).start()

    barrier = pltpu.get_barrier_semaphore()
    for j in range(1, n_tp):
        pl.semaphore_signal(
            barrier, inc=1, device_id={"tp": lax.rem(tp + j, n_tp)},
            device_id_type=pl.DeviceIdType.MESH,
        )
    for j in range(1, n_dp):
        pl.semaphore_signal(
            barrier, inc=1, device_id={"dp": lax.rem(dp + j, n_dp)},
            device_id_type=pl.DeviceIdType.MESH,
        )
    current[0, pl.ds(0, rows), :] = hidden_ref[...]
    for layer in range(layers):
        readout[layer] = jnp.zeros_like(readout[layer])
    pl.semaphore_wait(barrier, n_tp + n_dp - 2)

    def remote(src, dst, sems, index, axis, target):
        return pltpu.make_async_remote_copy(
            src_ref=src, dst_ref=dst,
            send_sem=sems.at[(0,) + index], recv_sem=sems.at[(1,) + index],
            device_id={axis: target}, device_id_type=pl.DeviceIdType.MESH,
        )

    pending = []

    for layer in range(layers):
        copies = []
        for j in range(1, n_tp):
            copy = remote(
                current.at[layer], gathered.at[layer, tp], gather_sems, (layer, j - 1),
                "tp", lax.rem(tp + j, n_tp),
            )
            copy.start()
            copies.append(copy)
        gathered[layer, tp] = current[layer]
        for copy in copies:
            copy.wait_recv()
        pending += copies
        widened = gathered[layer].reshape(n_tp * pad, width).astype(F32)
        scaled = (widened * gain_ref[layer, :][None, :]).astype(BF16)
        squares = jnp.sum(widened * widened, axis=1, keepdims=True)
        sq_send[layer] = jnp.broadcast_to(squares, (n_tp * pad, 128)).reshape(n_tp, pad, 128)
        sq_copies = []
        for j in range(1, n_dp):
            to = lax.rem(dp + j, n_dp)
            copy = remote(
                sq_send.at[layer, to], sq_recv.at[layer, j - 1], sq_sems, (layer, j - 1), "dp", to
            )
            copy.start()
            sq_copies.append(copy)

        part_copies = []
        p = 0
        for index, matrix in enumerate((wq, wk, wd, wv, wg)):
            load(index, layer).wait()
            for start in range(0, matrix.shape[2], piece):
                result = jnp.dot(
                    scaled, matrix[layer, :, pl.ds(start, piece)], preferred_element_type=F32
                )
                part_send[layer, p] = result.astype(BF16).reshape(n_dp, pad, piece)
                for j in range(1, n_dp):
                    to = lax.rem(dp + j, n_dp)
                    copy = remote(
                        part_send.at[layer, p, to], part_recv.at[layer, p, j - 1],
                        part_sems, (layer, p, j - 1), "dp", to,
                    )
                    copy.start()
                    part_copies.append(copy)
                p += 1
        pending += sq_copies + part_copies

        for copy in sq_copies:
            copy.wait_recv()
        total_squares = sq_send[layer, dp]
        for j in range(1, n_dp):
            total_squares = total_squares + sq_recv[layer, j - 1]
        inverse = lax.rsqrt(total_squares / d_model + EPSILON)[:, :1]

        def projected(p):
            for j in range(1, n_dp):
                part_copies[p * (n_dp - 1) + j - 1].wait_recv()
            total = part_send[layer, p, dp].astype(F32)
            for j in range(1, n_dp):
                total = total + part_recv[layer, p, j - 1].astype(F32)
            return total * inverse

        def projected_range(first, columns):
            got = [projected(first + i) for i in range(columns // piece)]
            return got[0] if len(got) == 1 else jnp.concatenate(got, axis=1)

        per_key = key_cols // piece
        per_value = value_cols // piece
        query = projected_range(0, key_cols)
        key = projected_range(per_key, key_cols) * head_key ** (-0.5)
        logits = projected_range(2 * per_key, key_cols)
        log_sigmoid = jnp.minimum(logits, 0.0) - jnp.log(1.0 + jnp.exp(-jnp.abs(logits)))
        decay_buf[layer, pl.ds(0, rows), :] = (
            log_sigmoid[:rows] / SOFTNESS + offset_ref[layer]
        )
        decay = jnp.exp(decay_buf[layer])
        stacked = jnp.concatenate(
            [query * decay, key, decay, jnp.zeros((128 - 3 * pad, key_cols), F32)], axis=0
        )
        turned[layer] = stacked.T.reshape(heads, head_key, 128)
        both = query * key
        for h in range(heads):
            own = both[:, h * head_key : (h + 1) * head_key]
            products[layer, h] = jnp.broadcast_to(
                jnp.sum(own, axis=1, keepdims=True), (pad, 128)
            )
        load(6, layer).wait()

        def read_head(h, _):
            columns = turned[layer, h]
            for b in range(rows):
                factor = jnp.broadcast_to(columns[:, b : b + 1], (head_key, value_channels))
                readout[layer, h, pl.ds(b, 1), :] = jnp.sum(
                    factor * state[layer, b, h], axis=0, keepdims=True
                )
            return 0

        lax.fori_loop(0, heads, read_head, 0)

        value_buf[layer] = projected_range(3 * per_key, value_cols)
        gate_buf[layer] = projected_range(3 * per_key + per_value, value_cols)
        for h in range(heads):
            span = slice(h * value_channels, (h + 1) * value_channels)
            got = readout[layer, h] + products[layer, h] * value_buf[layer, :, span]
            gate = gate_buf[layer, :, span]
            normed = got * lax.rsqrt(jnp.mean(got * got, axis=1, keepdims=True) + EPSILON)
            normed = normed * out_gain_ref[layer, span][None, :]
            gated_all[layer, dp, :, span] = (normed * (gate / (1.0 + jnp.exp(-gate)))).astype(BF16)

        copies = []
        for j in range(1, n_dp):
            copy = remote(
                gated_all.at[layer, dp], gated_all.at[layer, dp], gated_sems, (layer, j - 1),
                "dp", lax.rem(dp + j, n_dp),
            )
            copy.start()
            copies.append(copy)

        def renew_head(h, _):
            columns = turned[layer, h]
            values = value_buf[layer, :, pl.ds(pl.multiple_of(h * value_channels, value_channels), value_channels)]
            for b in range(rows):
                shape = (head_key, value_channels)
                keep = jnp.broadcast_to(columns[:, 2 * pad + b : 2 * pad + b + 1], shape)
                add = jnp.broadcast_to(columns[:, pad + b : pad + b + 1], shape)
                new_state_ref[layer, b, h] = keep * state[layer, b, h] + add * values[b : b + 1]
            return 0

        lax.fori_loop(0, heads, renew_head, 0)

        load(5, layer).wait()
        for copy in copies:
            copy.wait_recv()
        pending += copies

        gated = gated_all[layer].reshape(n_dp * pad, value_cols)
        mix_copies = []
        for p in range(mix_pieces):
            result = jnp.dot(
                gated, wo[layer, :, pl.ds(p * mix_piece, mix_piece)], preferred_element_type=F32
            )
            mix_send[layer, p] = result.astype(BF16).reshape(n_tp, pad, mix_piece)
            for j in range(1, n_tp):
                to = lax.rem(tp + j, n_tp)
                copy = remote(
                    mix_send.at[layer, p, to], mix_recv.at[layer, p, j - 1],
                    mix_sems, (layer, p, j - 1), "tp", to,
                )
                copy.start()
                mix_copies.append(copy)
        pending += mix_copies
        for p in range(mix_pieces):
            span = slice(p * mix_piece, (p + 1) * mix_piece)
            for j in range(1, n_tp):
                mix_copies[p * (n_tp - 1) + j - 1].wait_recv()
            total = mix_send[layer, p, tp].astype(F32)
            for j in range(1, n_tp):
                total = total + mix_recv[layer, p, j - 1].astype(F32)
            result = (current[layer, :, span].astype(F32) + total).astype(BF16)
            if layer + 1 < layers:
                current[layer + 1, :, span] = result
            else:
                hidden_out_ref[:, span] = result[:rows]

    for copy in pending:
        copy.wait_send()


def fused(
    n_tp, n_dp, hidden_in, input_norm_gain, w_query, w_key, w_decay, w_value, w_gate,
    out_gain, w_out, decay_offset, state,
):
    layers, rows, heads, head_key, value_channels = state.shape
    width = hidden_in.shape[1]
    pad = -(-rows // 16) * 16
    key_cols, value_cols = w_query.shape[2], w_value.shape[2]
    piece = min(512, key_cols)
    pieces = (3 * key_cols + 2 * value_cols) // piece
    mix_piece = min(512, width)
    mix_pieces = width // mix_piece
    vmem = pl.BlockSpec(memory_space=pltpu.VMEM)
    hbm = pl.BlockSpec(memory_space=pl.ANY)
    return pl.pallas_call(
        functools.partial(
            block_kernel, n_tp, n_dp, width * n_dp, head_key, value_channels
        ),
        out_shape=(
            jax.ShapeDtypeStruct(hidden_in.shape, BF16),
            pltpu.VMEM(state.shape, F32),
        ),
        in_specs=[vmem] * 4 + [hbm] * 7,
        out_specs=(vmem, vmem),
        scratch_shapes=[
            pltpu.VMEM(w_query.shape, BF16),
            pltpu.VMEM(w_key.shape, BF16),
            pltpu.VMEM(w_decay.shape, BF16),
            pltpu.VMEM(w_value.shape, BF16),
            pltpu.VMEM(w_gate.shape, BF16),
            pltpu.VMEM(w_out.shape, BF16),
            pltpu.VMEM(state.shape, F32),
            pltpu.VMEM((layers, pad, width), BF16),
            pltpu.VMEM((layers, n_tp, pad, width), BF16),
            pltpu.VMEM((layers, pieces, n_dp, pad, piece), BF16),
            pltpu.VMEM((layers, pieces, n_dp - 1, pad, piece), BF16),
            pltpu.VMEM((layers, n_dp, pad, 128), F32),
            pltpu.VMEM((layers, n_dp - 1, pad, 128), F32),
            pltpu.VMEM((layers, heads, head_key, 128), F32),
            pltpu.VMEM((layers, heads, pad, 128), F32),
            pltpu.VMEM((layers, pad, value_cols), F32),
            pltpu.VMEM((layers, pad, value_cols), F32),
            pltpu.VMEM((layers, pad, key_cols), F32),
            pltpu.VMEM((layers, heads, pad, value_channels), F32),
            pltpu.VMEM((layers, n_dp, pad, value_cols), BF16),
            pltpu.VMEM((layers, mix_pieces, n_tp, pad, mix_piece), BF16),
            pltpu.VMEM((layers, mix_pieces, n_tp - 1, pad, mix_piece), BF16),
            pltpu.SemaphoreType.DMA((7, layers)),
            pltpu.SemaphoreType.DMA((2, layers, n_tp - 1)),
            pltpu.SemaphoreType.DMA((2, layers, pieces, n_dp - 1)),
            pltpu.SemaphoreType.DMA((2, layers, n_dp - 1)),
            pltpu.SemaphoreType.DMA((2, layers, n_dp - 1)),
            pltpu.SemaphoreType.DMA((2, layers, mix_pieces, n_tp - 1)),
        ],
        compiler_params=pltpu.CompilerParams(
            collective_id=0, has_side_effects=True, vmem_limit_bytes=48 * 1024 * 1024
        ),
    )(
        hidden_in, input_norm_gain, out_gain, decay_offset,
        w_query, w_key, w_decay, w_value, w_gate, w_out, state,
    )


def plain(
    hidden_in, input_norm_gain, w_query, w_key, w_decay, w_value, w_gate,
    out_gain, w_out, decay_offset, state,
):
    layers, rows, heads, head_key, value_channels = state.shape
    key_cols, value_cols = w_query.shape[2], w_value.shape[2]
    d_model = hidden_in.shape[1] * lax.axis_size("dp")
    first = lax.axis_index("dp") * rows
    current, states = hidden_in, []
    for layer in range(layers):
        widened = lax.all_gather(current, "tp", axis=0, tiled=True).astype(F32)
        squares = lax.psum(jnp.sum(widened * widened, axis=1), "dp")
        scaled = (widened * input_norm_gain[layer][None, :]).astype(BF16)
        partial = jnp.concatenate(
            [
                jnp.dot(scaled, matrix[layer], preferred_element_type=F32)
                for matrix in (w_query, w_key, w_decay, w_value, w_gate)
            ],
            axis=1,
        ).astype(BF16)
        summed = lax.psum_scatter(partial, "dp", scatter_dimension=0, tiled=True).astype(F32)
        own = lax.dynamic_slice_in_dim(squares, first, rows)
        projected = summed * lax.rsqrt(own / d_model + EPSILON)[:, None]
        query, key, logits, value, gate = jnp.split(
            projected,
            [key_cols, 2 * key_cols, 3 * key_cols, 3 * key_cols + value_cols],
            axis=1,
        )
        decay = jnp.exp(jax.nn.log_sigmoid(logits) / SOFTNESS + decay_offset[layer])
        per_key, per_value = (rows, heads, head_key), (rows, heads, value_channels)
        fresh = (
            decay.reshape(per_key)[..., None] * state[layer]
            + (key * head_key ** (-0.5)).reshape(per_key)[..., None]
            * value.reshape(per_value)[:, :, None, :]
        )
        got = jnp.sum(query.reshape(per_key)[..., None] * fresh, axis=2)
        got = got * lax.rsqrt(jnp.mean(got * got, axis=2, keepdims=True) + EPSILON)
        got = got * out_gain[layer].reshape(heads, value_channels)[None]
        gated = (got * jax.nn.silu(gate.reshape(per_value))).reshape(rows, value_cols).astype(BF16)
        mixed = jnp.dot(
            lax.all_gather(gated, "dp", axis=0, tiled=True), w_out[layer],
            preferred_element_type=F32,
        ).astype(BF16)
        mine = lax.psum_scatter(mixed, "tp", scatter_dimension=0, tiled=True).astype(F32)
        current = (current.astype(F32) + mine).astype(BF16)
        states.append(fresh)
    return current, jnp.stack(states)


def solution(mesh):
    n_tp, n_dp = mesh.shape["tp"], mesh.shape["dp"]

    def per_device(hidden_in, *rest):
        state = rest[-1]
        aligned = rest[1].shape[2] % 128 == 0 and hidden_in.shape[1] % 128 == 0
        if n_tp > 1 and n_tp == n_dp and aligned and 3 * state.shape[1] <= 96:
            return fused(n_tp, n_dp, hidden_in, *rest)
        return plain(hidden_in, *rest)

    return jax.shard_map(
        per_device,
        mesh=mesh,
        in_specs=(
            P(("grp", "tp"), "dp"),
            P(None, "dp"),
            P(None, "dp", "tp"),
            P(None, "dp", "tp"),
            P(None, "dp", "tp"),
            P(None, "dp", "tp"),
            P(None, "dp", "tp"),
            P(None, "tp"),
            P(None, "tp", "dp"),
            P(None, ("grp", "dp"), "tp"),
            P(None, ("grp", "dp"), "tp", None, None),
        ),
        out_specs=(P(("grp", "tp"), "dp"), P(None, ("grp", "dp"), "tp", None, None)),
        check_vma=False,
    )
```

```python
import functools

import jax
import jax.numpy as jnp
from jax import lax
from jax.experimental import pallas as pl
from jax.experimental.pallas import tpu as pltpu
from jax.sharding import PartitionSpec as P

EPSILON = 1e-06
SOFTNESS = 16.0
F32 = jnp.float32
BF16 = jnp.bfloat16


def pack(block, rows):
    if block.shape[0] != 16 or rows > 12 or block.shape[1] % 256:
        return block
    half = block.shape[1] // 2
    tail = jnp.concatenate([block[8:12, :half], block[8:12, half:]], axis=0)
    return jnp.concatenate([block[:8], tail], axis=1)


def unpack(block, rows, columns):
    if block.shape[1] == columns:
        return block
    tail = jnp.concatenate([block[:4, columns:], block[4:, columns:]], axis=1)
    return jnp.concatenate([block[:, :columns], tail, jnp.zeros_like(tail)], axis=0)


def packed_shape(pad, rows, columns):
    if pad != 16 or rows > 12 or columns % 256:
        return pad, columns
    return 8, columns // 2 * 3


def block_kernel(
    n_tp, n_dp, d_model, head_key, value_channels, piece, mix_piece,
    hidden_ref, gain_ref, out_gain_ref, offset_ref,
    wq_hbm, wk_hbm, wd_hbm, wv_hbm, wg_hbm, wo_hbm, state_hbm,
    hidden_out_ref, new_state_ref,
    wq, wk, wd, wv, wg, wo, state,
    current, gathered, part_send, part_recv, sq_send, sq_recv,
    turned, products, value_buf, gate_buf, decay_buf, readout,
    gated_all, mix_send, mix_recv,
    load_sem, gather_sems, part_sems, sq_sems, gated_sems, mix_sems,
):
    layers, rows, heads = state.shape[0], state.shape[1], state.shape[2]
    pad = current.shape[1]
    width = current.shape[2]
    mix_pieces = mix_send.shape[1]
    key_cols = heads * head_key
    value_cols = heads * value_channels
    tp = lax.axis_index("tp")
    dp = lax.axis_index("dp")

    sources = (wq_hbm, wk_hbm, wd_hbm, wv_hbm, wg_hbm, wo_hbm, state_hbm)
    targets = (wq, wk, wd, wv, wg, wo, state)

    def load(index, layer):
        return pltpu.make_async_copy(
            sources[index].at[layer], targets[index].at[layer], load_sem.at[index, layer]
        )

    for layer in range(layers):
        for index in (0, 1, 2, 3, 4, 6, 5):
            load(index, layer).start()

    barrier = pltpu.get_barrier_semaphore()
    for j in range(1, n_tp):
        pl.semaphore_signal(
            barrier, inc=1, device_id={"tp": lax.rem(tp + j, n_tp)},
            device_id_type=pl.DeviceIdType.MESH,
        )
    for j in range(1, n_dp):
        pl.semaphore_signal(
            barrier, inc=1, device_id={"dp": lax.rem(dp + j, n_dp)},
            device_id_type=pl.DeviceIdType.MESH,
        )
    current[0, pl.ds(0, rows), :] = hidden_ref[...]
    for layer in range(layers):
        readout[layer] = jnp.zeros_like(readout[layer])
    pl.semaphore_wait(barrier, n_tp + n_dp - 2)

    def remote(src, dst, sems, index, axis, target):
        return pltpu.make_async_remote_copy(
            src_ref=src, dst_ref=dst,
            send_sem=sems.at[(0,) + index], recv_sem=sems.at[(1,) + index],
            device_id={axis: target}, device_id_type=pl.DeviceIdType.MESH,
        )

    pending = []

    for layer in range(layers):
        gathered[layer, tp] = pack(current[layer].astype(F32), rows).astype(BF16)
        copies = []
        for j in range(1, n_tp):
            copy = remote(
                gathered.at[layer, tp], gathered.at[layer, tp], gather_sems, (layer, j - 1),
                "tp", lax.rem(tp + j, n_tp),
            )
            copy.start()
            copies.append(copy)
        for copy in copies:
            copy.wait_recv()
        pending += copies
        widened = jnp.concatenate(
            [unpack(gathered[layer, s].astype(F32), rows, width) for s in range(n_tp)], axis=0
        )
        scaled = (widened * gain_ref[layer, :][None, :]).astype(BF16)
        squares = jnp.sum(widened * widened, axis=1, keepdims=True)
        sq_send[layer] = jnp.broadcast_to(squares, (n_tp * pad, 128)).reshape(n_tp, pad, 128)
        sq_copies = []
        for j in range(1, n_dp):
            to = lax.rem(dp + j, n_dp)
            copy = remote(
                sq_send.at[layer, to], sq_recv.at[layer, j - 1], sq_sems, (layer, j - 1), "dp", to
            )
            copy.start()
            sq_copies.append(copy)

        part_copies = []
        p = 0
        for index, matrix in enumerate((wq, wk, wd, wv, wg)):
            load(index, layer).wait()
            for start in range(0, matrix.shape[2], piece):
                result = jnp.dot(
                    scaled, matrix[layer, :, pl.ds(start, piece)], preferred_element_type=F32
                )
                for s in range(n_dp):
                    block = result[s * pad : (s + 1) * pad]
                    part_send[layer, p, s] = pack(block, rows).astype(BF16)
                for j in range(1, n_dp):
                    to = lax.rem(dp + j, n_dp)
                    copy = remote(
                        part_send.at[layer, p, to], part_recv.at[layer, p, j - 1],
                        part_sems, (layer, p, j - 1), "dp", to,
                    )
                    copy.start()
                    part_copies.append(copy)
                p += 1
        pending += sq_copies + part_copies

        for copy in sq_copies:
            copy.wait_recv()
        total_squares = sq_send[layer, dp]
        for j in range(1, n_dp):
            total_squares = total_squares + sq_recv[layer, j - 1]
        inverse = lax.rsqrt(total_squares / d_model + EPSILON)[:, :1]

        def projected(p):
            for j in range(1, n_dp):
                part_copies[p * (n_dp - 1) + j - 1].wait_recv()
            total = part_send[layer, p, dp].astype(F32)
            for j in range(1, n_dp):
                total = total + part_recv[layer, p, j - 1].astype(F32)
            return unpack(total, rows, piece) * inverse

        def projected_range(first, columns):
            got = [projected(first + i) for i in range(columns // piece)]
            return got[0] if len(got) == 1 else jnp.concatenate(got, axis=1)

        per_key = key_cols // piece
        per_value = value_cols // piece
        query = projected_range(0, key_cols)
        key = projected_range(per_key, key_cols) * head_key ** (-0.5)
        logits = projected_range(2 * per_key, key_cols)
        log_sigmoid = jnp.minimum(logits, 0.0) - jnp.log(1.0 + jnp.exp(-jnp.abs(logits)))
        decay_buf[layer, pl.ds(0, rows), :] = (
            log_sigmoid[:rows] / SOFTNESS + offset_ref[:, layer, :]
        )
        decay = jnp.exp(decay_buf[layer])
        stacked = jnp.concatenate(
            [query * decay, key, decay, jnp.zeros((128 - 3 * pad, key_cols), F32)], axis=0
        )
        turned[layer] = stacked.T.reshape(heads, head_key, 128)
        both = query * key
        for h in range(heads):
            own = both[:, h * head_key : (h + 1) * head_key]
            products[layer, h] = jnp.broadcast_to(
                jnp.sum(own, axis=1, keepdims=True), (pad, 128)
            )
        load(6, layer).wait()

        def read_head(h, _):
            columns = turned[layer, h]
            for b in range(rows):
                factor = jnp.broadcast_to(columns[:, b : b + 1], (head_key, value_channels))
                readout[layer, h, pl.ds(b, 1), :] = jnp.sum(
                    factor * state[layer, b, h], axis=0, keepdims=True
                )
            return 0

        lax.fori_loop(0, heads, read_head, 0)

        value_buf[layer] = projected_range(3 * per_key, value_cols)
        gate_buf[layer] = projected_range(3 * per_key + per_value, value_cols)
        gated_heads = []
        for h in range(heads):
            span = slice(h * value_channels, (h + 1) * value_channels)
            got = readout[layer, h] + products[layer, h] * value_buf[layer, :, span]
            gate = gate_buf[layer, :, span]
            normed = got * lax.rsqrt(jnp.mean(got * got, axis=1, keepdims=True) + EPSILON)
            normed = normed * out_gain_ref[layer, span][None, :]
            gated_heads.append(normed * (gate / (1.0 + jnp.exp(-gate))))
        gated_all[layer, dp] = pack(jnp.concatenate(gated_heads, axis=1), rows).astype(BF16)

        copies = []
        for j in range(1, n_dp):
            copy = remote(
                gated_all.at[layer, dp], gated_all.at[layer, dp], gated_sems, (layer, j - 1),
                "dp", lax.rem(dp + j, n_dp),
            )
            copy.start()
            copies.append(copy)

        def renew_head(h, _):
            columns = turned[layer, h]
            values = value_buf[layer, :, pl.ds(pl.multiple_of(h * value_channels, value_channels), value_channels)]
            for b in range(rows):
                shape = (head_key, value_channels)
                keep = jnp.broadcast_to(columns[:, 2 * pad + b : 2 * pad + b + 1], shape)
                add = jnp.broadcast_to(columns[:, pad + b : pad + b + 1], shape)
                new_state_ref[layer, b, h] = keep * state[layer, b, h] + add * values[b : b + 1]
            return 0

        lax.fori_loop(0, heads, renew_head, 0)

        load(5, layer).wait()
        for copy in copies:
            copy.wait_recv()
        pending += copies

        gated = jnp.concatenate(
            [
                unpack(gated_all[layer, s].astype(F32), rows, value_cols).astype(BF16)
                for s in range(n_dp)
            ],
            axis=0,
        )
        mix_copies = []
        for p in range(mix_pieces):
            result = jnp.dot(
                gated, wo[layer, :, pl.ds(p * mix_piece, mix_piece)], preferred_element_type=F32
            )
            for s in range(n_tp):
                block = result[s * pad : (s + 1) * pad]
                mix_send[layer, p, s] = pack(block, rows).astype(BF16)
            for j in range(1, n_tp):
                to = lax.rem(tp + j, n_tp)
                copy = remote(
                    mix_send.at[layer, p, to], mix_recv.at[layer, p, j - 1],
                    mix_sems, (layer, p, j - 1), "tp", to,
                )
                copy.start()
                mix_copies.append(copy)
        pending += mix_copies
        for p in range(mix_pieces):
            span = slice(p * mix_piece, (p + 1) * mix_piece)
            for j in range(1, n_tp):
                mix_copies[p * (n_tp - 1) + j - 1].wait_recv()
            total = mix_send[layer, p, tp].astype(F32)
            for j in range(1, n_tp):
                total = total + mix_recv[layer, p, j - 1].astype(F32)
            total = unpack(total, rows, mix_piece)
            result = (current[layer, :, span].astype(F32) + total).astype(BF16)
            if layer + 1 < layers:
                current[layer + 1, :, span] = result
            else:
                hidden_out_ref[:, span] = result[:rows]

    for copy in pending:
        copy.wait_send()


def fused(
    n_tp, n_dp, hidden_in, input_norm_gain, w_query, w_key, w_decay, w_value, w_gate,
    out_gain, w_out, decay_offset, state,
):
    layers, rows, heads, head_key, value_channels = state.shape
    width = hidden_in.shape[1]
    pad = -(-rows // 16) * 16
    key_cols, value_cols = w_query.shape[2], w_value.shape[2]
    piece = min(512, key_cols)
    pieces = (3 * key_cols + 2 * value_cols) // piece
    mix_piece = min(512, width)
    mix_pieces = width // mix_piece
    part_shape = packed_shape(pad, rows, piece)
    mix_shape = packed_shape(pad, rows, mix_piece)
    vmem = pl.BlockSpec(memory_space=pltpu.VMEM)
    hbm = pl.BlockSpec(memory_space=pl.ANY)
    return pl.pallas_call(
        functools.partial(
            block_kernel, n_tp, n_dp, width * n_dp, head_key, value_channels,
            piece, mix_piece,
        ),
        out_shape=(
            jax.ShapeDtypeStruct(hidden_in.shape, BF16),
            pltpu.VMEM(state.shape, F32),
        ),
        in_specs=[vmem] * 4 + [hbm] * 7,
        out_specs=(vmem, vmem),
        scratch_shapes=[
            pltpu.VMEM(w_query.shape, BF16),
            pltpu.VMEM(w_key.shape, BF16),
            pltpu.VMEM(w_decay.shape, BF16),
            pltpu.VMEM(w_value.shape, BF16),
            pltpu.VMEM(w_gate.shape, BF16),
            pltpu.VMEM(w_out.shape, BF16),
            pltpu.VMEM(state.shape, F32),
            pltpu.VMEM((layers, pad, width), BF16),
            pltpu.VMEM((layers, n_tp) + packed_shape(pad, rows, width), BF16),
            pltpu.VMEM((layers, pieces, n_dp) + part_shape, BF16),
            pltpu.VMEM((layers, pieces, n_dp - 1) + part_shape, BF16),
            pltpu.VMEM((layers, n_dp, pad, 128), F32),
            pltpu.VMEM((layers, n_dp - 1, pad, 128), F32),
            pltpu.VMEM((layers, heads, head_key, 128), F32),
            pltpu.VMEM((layers, heads, pad, 128), F32),
            pltpu.VMEM((layers, pad, value_cols), F32),
            pltpu.VMEM((layers, pad, value_cols), F32),
            pltpu.VMEM((layers, pad, key_cols), F32),
            pltpu.VMEM((layers, heads, pad, value_channels), F32),
            pltpu.VMEM((layers, n_dp) + packed_shape(pad, rows, value_cols), BF16),
            pltpu.VMEM((layers, mix_pieces, n_tp) + mix_shape, BF16),
            pltpu.VMEM((layers, mix_pieces, n_tp - 1) + mix_shape, BF16),
            pltpu.SemaphoreType.DMA((7, layers)),
            pltpu.SemaphoreType.DMA((2, layers, n_tp - 1)),
            pltpu.SemaphoreType.DMA((2, layers, pieces, n_dp - 1)),
            pltpu.SemaphoreType.DMA((2, layers, n_dp - 1)),
            pltpu.SemaphoreType.DMA((2, layers, n_dp - 1)),
            pltpu.SemaphoreType.DMA((2, layers, mix_pieces, n_tp - 1)),
        ],
        compiler_params=pltpu.CompilerParams(
            collective_id=0, has_side_effects=True, vmem_limit_bytes=48 * 1024 * 1024
        ),
    )(
        hidden_in, input_norm_gain, out_gain, decay_offset.transpose(1, 0, 2),
        w_query, w_key, w_decay, w_value, w_gate, w_out, state,
    )


def plain(
    hidden_in, input_norm_gain, w_query, w_key, w_decay, w_value, w_gate,
    out_gain, w_out, decay_offset, state,
):
    layers, rows, heads, head_key, value_channels = state.shape
    key_cols, value_cols = w_query.shape[2], w_value.shape[2]
    d_model = hidden_in.shape[1] * lax.axis_size("dp")
    first = lax.axis_index("dp") * rows
    current, states = hidden_in, []
    for layer in range(layers):
        widened = lax.all_gather(current, "tp", axis=0, tiled=True).astype(F32)
        squares = lax.psum(jnp.sum(widened * widened, axis=1), "dp")
        scaled = (widened * input_norm_gain[layer][None, :]).astype(BF16)
        partial = jnp.concatenate(
            [
                jnp.dot(scaled, matrix[layer], preferred_element_type=F32)
                for matrix in (w_query, w_key, w_decay, w_value, w_gate)
            ],
            axis=1,
        ).astype(BF16)
        summed = lax.psum_scatter(partial, "dp", scatter_dimension=0, tiled=True).astype(F32)
        own = lax.dynamic_slice_in_dim(squares, first, rows)
        projected = summed * lax.rsqrt(own / d_model + EPSILON)[:, None]
        query, key, logits, value, gate = jnp.split(
            projected,
            [key_cols, 2 * key_cols, 3 * key_cols, 3 * key_cols + value_cols],
            axis=1,
        )
        decay = jnp.exp(jax.nn.log_sigmoid(logits) / SOFTNESS + decay_offset[layer])
        per_key, per_value = (rows, heads, head_key), (rows, heads, value_channels)
        fresh = (
            decay.reshape(per_key)[..., None] * state[layer]
            + (key * head_key ** (-0.5)).reshape(per_key)[..., None]
            * value.reshape(per_value)[:, :, None, :]
        )
        got = jnp.sum(query.reshape(per_key)[..., None] * fresh, axis=2)
        got = got * lax.rsqrt(jnp.mean(got * got, axis=2, keepdims=True) + EPSILON)
        got = got * out_gain[layer].reshape(heads, value_channels)[None]
        gated = (got * jax.nn.silu(gate.reshape(per_value))).reshape(rows, value_cols).astype(BF16)
        mixed = jnp.dot(
            lax.all_gather(gated, "dp", axis=0, tiled=True), w_out[layer],
            preferred_element_type=F32,
        ).astype(BF16)
        mine = lax.psum_scatter(mixed, "tp", scatter_dimension=0, tiled=True).astype(F32)
        current = (current.astype(F32) + mine).astype(BF16)
        states.append(fresh)
    return current, jnp.stack(states)


def solution(mesh):
    n_tp, n_dp = mesh.shape["tp"], mesh.shape["dp"]

    def per_device(hidden_in, *rest):
        state = rest[-1]
        aligned = rest[1].shape[2] % 128 == 0 and hidden_in.shape[1] % 128 == 0
        if n_tp > 1 and n_tp == n_dp and aligned and 3 * state.shape[1] <= 96:
            return fused(n_tp, n_dp, hidden_in, *rest)
        return plain(hidden_in, *rest)

    return jax.shard_map(
        per_device,
        mesh=mesh,
        in_specs=(
            P(("grp", "tp"), "dp"),
            P(None, "dp"),
            P(None, "dp", "tp"),
            P(None, "dp", "tp"),
            P(None, "dp", "tp"),
            P(None, "dp", "tp"),
            P(None, "dp", "tp"),
            P(None, "tp"),
            P(None, "tp", "dp"),
            P(None, ("grp", "dp"), "tp"),
            P(None, ("grp", "dp"), "tp", None, None),
        ),
        out_specs=(P(("grp", "tp"), "dp"), P(None, ("grp", "dp"), "tp", None, None)),
        check_vma=False,
    )
```

```python
import functools

import jax
import jax.numpy as jnp
from jax import lax
from jax.experimental import pallas as pl
from jax.experimental.pallas import tpu as pltpu
from jax.sharding import PartitionSpec as P

EPSILON = 1e-06
SOFTNESS = 16.0
F32 = jnp.float32
BF16 = jnp.bfloat16


def pack(block, rows):
    if block.shape[0] != 16 or rows > 12 or block.shape[1] % 256:
        return block
    half = block.shape[1] // 2
    tail = jnp.concatenate([block[8:12, :half], block[8:12, half:]], axis=0)
    return jnp.concatenate([block[:8], tail], axis=1)


def unpack(block, rows, columns):
    if block.shape[1] == columns:
        return block
    tail = jnp.concatenate([block[:4, columns:], block[4:, columns:]], axis=1)
    return jnp.concatenate([block[:, :columns], tail, jnp.zeros_like(tail)], axis=0)


def packed_shape(pad, rows, columns):
    if pad != 16 or rows > 12 or columns % 256:
        return pad, columns
    return 8, columns // 2 * 3


def block_kernel(
    n_tp, n_dp, d_model, head_key, value_channels, piece, mix_piece,
    hidden_ref, gain_ref, out_gain_ref, offset_ref,
    wq_hbm, wk_hbm, wd_hbm, wv_hbm, wg_hbm, wo_hbm, state_hbm,
    hidden_out_ref, new_state_ref,
    wq, wk, wd, wv, wg, wo, state,
    current, gathered, part_send, part_recv, sq_send, sq_recv,
    turned, products, value_buf, gate_buf, decay_buf, readout,
    gated_all, mix_send, mix_recv,
    load_sem, gather_sems, part_sems, sq_sems, gated_sems, mix_sems,
):
    layers, rows, heads = state.shape[0], state.shape[1], state.shape[2]
    pad = current.shape[1]
    mix_pieces = mix_send.shape[1]
    key_cols = heads * head_key
    value_cols = heads * value_channels
    tp = lax.axis_index("tp")
    dp = lax.axis_index("dp")

    sources = (wq_hbm, wk_hbm, wd_hbm, wv_hbm, wg_hbm, wo_hbm, state_hbm)
    targets = (wq, wk, wd, wv, wg, wo, state)

    def load(index, layer):
        return pltpu.make_async_copy(
            sources[index].at[layer], targets[index].at[layer], load_sem.at[index, layer]
        )

    for layer in range(layers):
        for index in (0, 1, 2, 3, 4, 6, 5):
            load(index, layer).start()

    barrier = pltpu.get_barrier_semaphore()
    for j in range(1, n_tp):
        pl.semaphore_signal(
            barrier, inc=1, device_id={"tp": lax.rem(tp + j, n_tp)},
            device_id_type=pl.DeviceIdType.MESH,
        )
    for j in range(1, n_dp):
        pl.semaphore_signal(
            barrier, inc=1, device_id={"dp": lax.rem(dp + j, n_dp)},
            device_id_type=pl.DeviceIdType.MESH,
        )
    current[0, pl.ds(0, rows), :] = hidden_ref[...]
    for layer in range(layers):
        readout[layer] = jnp.zeros_like(readout[layer])
    pl.semaphore_wait(barrier, n_tp + n_dp - 2)

    def remote(src, dst, sems, index, axis, target):
        return pltpu.make_async_remote_copy(
            src_ref=src, dst_ref=dst,
            send_sem=sems.at[(0,) + index], recv_sem=sems.at[(1,) + index],
            device_id={axis: target}, device_id_type=pl.DeviceIdType.MESH,
        )

    pending = []

    def send_features(layer, p):
        block = current[layer, :, pl.ds(p * mix_piece, mix_piece)].astype(F32)
        gathered[layer, p, tp] = pack(block, rows).astype(BF16)
        sent = []
        for j in range(1, n_tp):
            copy = remote(
                gathered.at[layer, p, tp], gathered.at[layer, p, tp], gather_sems,
                (layer, p, j - 1), "tp", lax.rem(tp + j, n_tp),
            )
            copy.start()
            sent.append(copy)
        return sent

    feature_copies = []
    for p in range(mix_pieces):
        feature_copies += send_features(0, p)

    for layer in range(layers):
        copies = feature_copies
        feature_copies = []
        for copy in copies:
            copy.wait_recv()
        pending += copies
        widened = jnp.concatenate(
            [
                jnp.concatenate(
                    [
                        unpack(gathered[layer, p, s].astype(F32), rows, mix_piece)
                        for p in range(mix_pieces)
                    ],
                    axis=1,
                )
                for s in range(n_tp)
            ],
            axis=0,
        )
        scaled = (widened * gain_ref[layer, :][None, :]).astype(BF16)
        squares = jnp.sum(widened * widened, axis=1, keepdims=True)
        sq_send[layer] = jnp.broadcast_to(squares, (n_tp * pad, 128)).reshape(n_tp, pad, 128)
        sq_copies = []
        for j in range(1, n_dp):
            to = lax.rem(dp + j, n_dp)
            copy = remote(
                sq_send.at[layer, to], sq_recv.at[layer, j - 1], sq_sems, (layer, j - 1), "dp", to
            )
            copy.start()
            sq_copies.append(copy)

        part_copies = []
        p = 0
        for index, matrix in enumerate((wq, wk, wd, wv, wg)):
            load(index, layer).wait()
            for start in range(0, matrix.shape[2], piece):
                result = jnp.dot(
                    scaled, matrix[layer, :, pl.ds(start, piece)], preferred_element_type=F32
                )
                for s in range(n_dp):
                    block = result[s * pad : (s + 1) * pad]
                    part_send[layer, p, s] = pack(block, rows).astype(BF16)
                for j in range(1, n_dp):
                    to = lax.rem(dp + j, n_dp)
                    copy = remote(
                        part_send.at[layer, p, to], part_recv.at[layer, p, j - 1],
                        part_sems, (layer, p, j - 1), "dp", to,
                    )
                    copy.start()
                    part_copies.append(copy)
                p += 1
        pending += sq_copies + part_copies

        for copy in sq_copies:
            copy.wait_recv()
        total_squares = sq_send[layer, dp]
        for j in range(1, n_dp):
            total_squares = total_squares + sq_recv[layer, j - 1]
        inverse = lax.rsqrt(total_squares / d_model + EPSILON)[:, :1]

        def projected(p):
            for j in range(1, n_dp):
                part_copies[p * (n_dp - 1) + j - 1].wait_recv()
            total = part_send[layer, p, dp].astype(F32)
            for j in range(1, n_dp):
                total = total + part_recv[layer, p, j - 1].astype(F32)
            return unpack(total, rows, piece) * inverse

        def projected_range(first, columns):
            got = [projected(first + i) for i in range(columns // piece)]
            return got[0] if len(got) == 1 else jnp.concatenate(got, axis=1)

        per_key = key_cols // piece
        per_value = value_cols // piece
        query = projected_range(0, key_cols)
        key = projected_range(per_key, key_cols) * head_key ** (-0.5)
        logits = projected_range(2 * per_key, key_cols)
        log_sigmoid = jnp.minimum(logits, 0.0) - jnp.log(1.0 + jnp.exp(-jnp.abs(logits)))
        decay_buf[layer, pl.ds(0, rows), :] = (
            log_sigmoid[:rows] / SOFTNESS + offset_ref[:, layer, :]
        )
        decay = jnp.exp(decay_buf[layer])
        stacked = jnp.concatenate(
            [query * decay, key, decay, jnp.zeros((128 - 3 * pad, key_cols), F32)], axis=0
        )
        turned[layer] = stacked.T.reshape(heads, head_key, 128)
        both = query * key
        for h in range(heads):
            own = both[:, h * head_key : (h + 1) * head_key]
            products[layer, h] = jnp.broadcast_to(
                jnp.sum(own, axis=1, keepdims=True), (pad, 128)
            )
        load(6, layer).wait()

        def read_head(h, _):
            columns = turned[layer, h]
            for b in range(rows):
                factor = jnp.broadcast_to(columns[:, b : b + 1], (head_key, value_channels))
                readout[layer, h, pl.ds(b, 1), :] = jnp.sum(
                    factor * state[layer, b, h], axis=0, keepdims=True
                )
            return 0

        lax.fori_loop(0, heads, read_head, 0)

        value_buf[layer] = projected_range(3 * per_key, value_cols)
        gate_buf[layer] = projected_range(3 * per_key + per_value, value_cols)
        gated_heads = []
        for h in range(heads):
            span = slice(h * value_channels, (h + 1) * value_channels)
            got = readout[layer, h] + products[layer, h] * value_buf[layer, :, span]
            gate = gate_buf[layer, :, span]
            normed = got * lax.rsqrt(jnp.mean(got * got, axis=1, keepdims=True) + EPSILON)
            normed = normed * out_gain_ref[layer, span][None, :]
            gated_heads.append(normed * (gate / (1.0 + jnp.exp(-gate))))
        gated_all[layer, dp] = pack(jnp.concatenate(gated_heads, axis=1), rows).astype(BF16)

        copies = []
        for j in range(1, n_dp):
            copy = remote(
                gated_all.at[layer, dp], gated_all.at[layer, dp], gated_sems, (layer, j - 1),
                "dp", lax.rem(dp + j, n_dp),
            )
            copy.start()
            copies.append(copy)

        def renew_head(h, _):
            columns = turned[layer, h]
            values = value_buf[layer, :, pl.ds(pl.multiple_of(h * value_channels, value_channels), value_channels)]
            for b in range(rows):
                shape = (head_key, value_channels)
                keep = jnp.broadcast_to(columns[:, 2 * pad + b : 2 * pad + b + 1], shape)
                add = jnp.broadcast_to(columns[:, pad + b : pad + b + 1], shape)
                new_state_ref[layer, b, h] = keep * state[layer, b, h] + add * values[b : b + 1]
            return 0

        lax.fori_loop(0, heads, renew_head, 0)

        load(5, layer).wait()
        for copy in copies:
            copy.wait_recv()
        pending += copies

        gated = jnp.concatenate(
            [
                unpack(gated_all[layer, s].astype(F32), rows, value_cols).astype(BF16)
                for s in range(n_dp)
            ],
            axis=0,
        )
        mix_copies = []
        for p in range(mix_pieces):
            result = jnp.dot(
                gated, wo[layer, :, pl.ds(p * mix_piece, mix_piece)], preferred_element_type=F32
            )
            for s in range(n_tp):
                block = result[s * pad : (s + 1) * pad]
                mix_send[layer, p, s] = pack(block, rows).astype(BF16)
            for j in range(1, n_tp):
                to = lax.rem(tp + j, n_tp)
                copy = remote(
                    mix_send.at[layer, p, to], mix_recv.at[layer, p, j - 1],
                    mix_sems, (layer, p, j - 1), "tp", to,
                )
                copy.start()
                mix_copies.append(copy)
        pending += mix_copies
        for p in range(mix_pieces):
            span = slice(p * mix_piece, (p + 1) * mix_piece)
            for j in range(1, n_tp):
                mix_copies[p * (n_tp - 1) + j - 1].wait_recv()
            total = mix_send[layer, p, tp].astype(F32)
            for j in range(1, n_tp):
                total = total + mix_recv[layer, p, j - 1].astype(F32)
            total = unpack(total, rows, mix_piece)
            result = (current[layer, :, span].astype(F32) + total).astype(BF16)
            if layer + 1 < layers:
                current[layer + 1, :, span] = result
                feature_copies += send_features(layer + 1, p)
            else:
                hidden_out_ref[:, span] = result[:rows]

    for copy in pending:
        copy.wait_send()


def fused(
    n_tp, n_dp, hidden_in, input_norm_gain, w_query, w_key, w_decay, w_value, w_gate,
    out_gain, w_out, decay_offset, state,
):
    layers, rows, heads, head_key, value_channels = state.shape
    width = hidden_in.shape[1]
    pad = -(-rows // 16) * 16
    key_cols, value_cols = w_query.shape[2], w_value.shape[2]
    piece = min(512, key_cols)
    pieces = (3 * key_cols + 2 * value_cols) // piece
    mix_piece = min(512, width)
    mix_pieces = width // mix_piece
    part_shape = packed_shape(pad, rows, piece)
    mix_shape = packed_shape(pad, rows, mix_piece)
    vmem = pl.BlockSpec(memory_space=pltpu.VMEM)
    hbm = pl.BlockSpec(memory_space=pl.ANY)
    return pl.pallas_call(
        functools.partial(
            block_kernel, n_tp, n_dp, width * n_dp, head_key, value_channels,
            piece, mix_piece,
        ),
        out_shape=(
            jax.ShapeDtypeStruct(hidden_in.shape, BF16),
            pltpu.VMEM(state.shape, F32),
        ),
        in_specs=[vmem] * 4 + [hbm] * 7,
        out_specs=(vmem, vmem),
        scratch_shapes=[
            pltpu.VMEM(w_query.shape, BF16),
            pltpu.VMEM(w_key.shape, BF16),
            pltpu.VMEM(w_decay.shape, BF16),
            pltpu.VMEM(w_value.shape, BF16),
            pltpu.VMEM(w_gate.shape, BF16),
            pltpu.VMEM(w_out.shape, BF16),
            pltpu.VMEM(state.shape, F32),
            pltpu.VMEM((layers, pad, width), BF16),
            pltpu.VMEM((layers, mix_pieces, n_tp) + mix_shape, BF16),
            pltpu.VMEM((layers, pieces, n_dp) + part_shape, BF16),
            pltpu.VMEM((layers, pieces, n_dp - 1) + part_shape, BF16),
            pltpu.VMEM((layers, n_dp, pad, 128), F32),
            pltpu.VMEM((layers, n_dp - 1, pad, 128), F32),
            pltpu.VMEM((layers, heads, head_key, 128), F32),
            pltpu.VMEM((layers, heads, pad, 128), F32),
            pltpu.VMEM((layers, pad, value_cols), F32),
            pltpu.VMEM((layers, pad, value_cols), F32),
            pltpu.VMEM((layers, pad, key_cols), F32),
            pltpu.VMEM((layers, heads, pad, value_channels), F32),
            pltpu.VMEM((layers, n_dp) + packed_shape(pad, rows, value_cols), BF16),
            pltpu.VMEM((layers, mix_pieces, n_tp) + mix_shape, BF16),
            pltpu.VMEM((layers, mix_pieces, n_tp - 1) + mix_shape, BF16),
            pltpu.SemaphoreType.DMA((7, layers)),
            pltpu.SemaphoreType.DMA((2, layers, mix_pieces, n_tp - 1)),
            pltpu.SemaphoreType.DMA((2, layers, pieces, n_dp - 1)),
            pltpu.SemaphoreType.DMA((2, layers, n_dp - 1)),
            pltpu.SemaphoreType.DMA((2, layers, n_dp - 1)),
            pltpu.SemaphoreType.DMA((2, layers, mix_pieces, n_tp - 1)),
        ],
        compiler_params=pltpu.CompilerParams(
            collective_id=0, has_side_effects=True, vmem_limit_bytes=48 * 1024 * 1024
        ),
    )(
        hidden_in, input_norm_gain, out_gain, decay_offset.transpose(1, 0, 2),
        w_query, w_key, w_decay, w_value, w_gate, w_out, state,
    )


def plain(
    hidden_in, input_norm_gain, w_query, w_key, w_decay, w_value, w_gate,
    out_gain, w_out, decay_offset, state,
):
    layers, rows, heads, head_key, value_channels = state.shape
    key_cols, value_cols = w_query.shape[2], w_value.shape[2]
    d_model = hidden_in.shape[1] * lax.axis_size("dp")
    first = lax.axis_index("dp") * rows
    current, states = hidden_in, []
    for layer in range(layers):
        widened = lax.all_gather(current, "tp", axis=0, tiled=True).astype(F32)
        squares = lax.psum(jnp.sum(widened * widened, axis=1), "dp")
        scaled = (widened * input_norm_gain[layer][None, :]).astype(BF16)
        partial = jnp.concatenate(
            [
                jnp.dot(scaled, matrix[layer], preferred_element_type=F32)
                for matrix in (w_query, w_key, w_decay, w_value, w_gate)
            ],
            axis=1,
        ).astype(BF16)
        summed = lax.psum_scatter(partial, "dp", scatter_dimension=0, tiled=True).astype(F32)
        own = lax.dynamic_slice_in_dim(squares, first, rows)
        projected = summed * lax.rsqrt(own / d_model + EPSILON)[:, None]
        query, key, logits, value, gate = jnp.split(
            projected,
            [key_cols, 2 * key_cols, 3 * key_cols, 3 * key_cols + value_cols],
            axis=1,
        )
        decay = jnp.exp(jax.nn.log_sigmoid(logits) / SOFTNESS + decay_offset[layer])
        per_key, per_value = (rows, heads, head_key), (rows, heads, value_channels)
        fresh = (
            decay.reshape(per_key)[..., None] * state[layer]
            + (key * head_key ** (-0.5)).reshape(per_key)[..., None]
            * value.reshape(per_value)[:, :, None, :]
        )
        got = jnp.sum(query.reshape(per_key)[..., None] * fresh, axis=2)
        got = got * lax.rsqrt(jnp.mean(got * got, axis=2, keepdims=True) + EPSILON)
        got = got * out_gain[layer].reshape(heads, value_channels)[None]
        gated = (got * jax.nn.silu(gate.reshape(per_value))).reshape(rows, value_cols).astype(BF16)
        mixed = jnp.dot(
            lax.all_gather(gated, "dp", axis=0, tiled=True), w_out[layer],
            preferred_element_type=F32,
        ).astype(BF16)
        mine = lax.psum_scatter(mixed, "tp", scatter_dimension=0, tiled=True).astype(F32)
        current = (current.astype(F32) + mine).astype(BF16)
        states.append(fresh)
    return current, jnp.stack(states)


def solution(mesh):
    n_tp, n_dp = mesh.shape["tp"], mesh.shape["dp"]

    def per_device(hidden_in, *rest):
        state = rest[-1]
        aligned = rest[1].shape[2] % 128 == 0 and hidden_in.shape[1] % 128 == 0
        if n_tp > 1 and n_tp == n_dp and aligned and 3 * state.shape[1] <= 96:
            return fused(n_tp, n_dp, hidden_in, *rest)
        return plain(hidden_in, *rest)

    return jax.shard_map(
        per_device,
        mesh=mesh,
        in_specs=(
            P(("grp", "tp"), "dp"),
            P(None, "dp"),
            P(None, "dp", "tp"),
            P(None, "dp", "tp"),
            P(None, "dp", "tp"),
            P(None, "dp", "tp"),
            P(None, "dp", "tp"),
            P(None, "tp"),
            P(None, "tp", "dp"),
            P(None, ("grp", "dp"), "tp"),
            P(None, ("grp", "dp"), "tp", None, None),
        ),
        out_specs=(P(("grp", "tp"), "dp"), P(None, ("grp", "dp"), "tp", None, None)),
        check_vma=False,
    )
```
